32 devices in a mesh: ep: 8 (over z, y), tp: 4 (over x, core).
Axes of the slice: x: 2, y: 2, z: 4, core: 2. Of those that a mesh axis runs over, the one named last changes fastest.
Arguments:
- mixer_in: bfloat16 [3072, 2048], P(('ep', 'tp')), may hold values from -8192 to 8192
- mixer_gain: float32 [2048], replicated, may hold values from 0.1 to 1.9
- query_weight: bfloat16 [2048, 512], P(None, 'tp'), may hold values from -4 to 4
- key_weight: bfloat16 [2048, 512], P(None, 'tp'), may hold values from -4 to 4
- value_weight: bfloat16 [2048, 512], P(None, 'tp'), may hold values from -0.125 to 0.125
- head_lambda: float32 [4], P('tp'), may hold values from 0.3 to 0.8
- head_gain: float32 [128], replicated, may hold values from 0.1 to 1.9
- out_weight: bfloat16 [512, 2048], P('tp'), may hold values from -0.25 to 0.25
- expert_in: bfloat16 [3072, 2048], P(('ep', 'tp')), may hold values from -6 to 6
- expert_gain: float32 [2048], replicated, may hold values from 0.1 to 1.9
- routes: int32 [3072, 2], P(('ep', 'tp')), may hold values from 0 to 7, all different within a row; in each aligned block of 96 rows (0 to 95, 96 to 191, ...) at most 48 rows name the same one
- route_weights: float32 [3072, 2], P(('ep', 'tp')), may hold values from 0.1 to 1
- gate_weight: bfloat16 [8, 2048, 512], P('ep'), may hold values from -0.125 to 0.125
- up_weight: bfloat16 [8, 2048, 512], P('ep'), may hold values from -0.125 to 0.125
- down_weight: bfloat16 [8, 512, 2048], P('ep'), may hold values from -0.25 to 0.25
- shared_gate: bfloat16 [2048, 512], P(None, 'tp'), may hold values from -0.125 to 0.125
- shared_up: bfloat16 [2048, 512], P(None, 'tp'), may hold values from -0.125 to 0.125
- shared_down: bfloat16 [512, 2048], P('tp'), may hold values from -0.25 to 0.25
Outputs:
- mixed_out: bfloat16 [3072, 2048], P(('ep', 'tp'))
- expert_out: bfloat16 [3072, 2048], P(('ep', 'tp'))
The draws below stay inside these ranges and needn't reach their ends.
Inputs may be any that keep to these rules, and one draw needn't show every extreme that they name: `routes`: each row names 2 different experts. Among the 96 rows of one device no expert is named more than 48 times, and in every draw some device's rows name some expert exactly 48 times.
All inputs are finite; a program needn't handle non-finite values.
Results may differ from the reference program's by a relative error of at most 0.013.
The reference program's roundings to bfloat16 on the way count: a program that leaves them out, or rounds other values in their place, can miss the bound.
Values may be sent and summed in bfloat16 or wider, within the bound.
A program may use at most 128 MiB of HBM per device.

```python
import math
from functools import partial
import jax
import jax.numpy as jnp
import numpy as np
from jax import lax

D = 2048
HEADS = 4
HALF = 64
VDIM = 128
FE = 512
FS = 512
TOPK = 2
TOK_DEV = 96
TOKENS = 3072
EXPERTS = 8
CAP = 48
N_TP = 4


def draw_mixer_in(key, part):
    key_base = jax.random.fold_in(jax.random.fold_in(key, 31), 0)
    base = jnp.clip(jax.random.normal(key_base, (TOKENS, D), jnp.float32), -6.0, 6.0)
    return base.astype(jnp.bfloat16)


def draw_query_weight(key, part):
    normal_part = jax.random.normal(jax.random.fold_in(key, 21), (D, HEADS * 2 * HALF), jnp.float32)
    base = jnp.clip(normal_part, -4.0, 4.0) * math.sqrt(3.0 / D)
    return base.astype(jnp.bfloat16)


def draw_key_weight(key, part):
    normal_part = jax.random.normal(jax.random.fold_in(key, 22), (D, HEADS * 2 * HALF), jnp.float32)
    base = jnp.clip(normal_part, -4.0, 4.0) * math.sqrt(1.0 / D)
    return base.astype(jnp.bfloat16)


def steps_of(stream_key, dims, pieces, low, largest):
    factor_of, own = 1.0, jax.random.fold_in(stream_key, 6)
    for dim, shards_of in pieces:
        draws = jnp.exp(jax.random.uniform(jax.random.fold_in(own, dim), (shards_of,), jnp.float32, low / len(pieces), largest / len(pieces)))
        factor_of = factor_of * jnp.repeat(draws, dims[dim] // shards_of).reshape([-1 if axis == dim else 1 for axis in range(len(dims))])
    return factor_of


def assign_block(stream_key, own, number, rows, amount, top, limit, slope):
    sequence = jax.random.permutation(stream_key, amount)
    crowded, common = load_shares(amount, rows * top, limit, slope, True), load_shares(amount, rows * top, limit, slope, False)
    places = jnp.arange(amount)

    def named(sizes, turn):
        used = int((sizes > 0).sum())
        fixed = max(1, used // 4)
        passed = fixed + (places - fixed + turn * (used - fixed)) % max(1, amount - fixed)
        return jnp.zeros((amount,), jnp.int32).at[sequence[jnp.where(places < fixed, places, passed)]].set(jnp.asarray(sizes, jnp.int32))

    sizes = jnp.where(number % 4 == 0, named(crowded, number // 4), named(common, number - number // 4 - 1))
    mixed = jax.random.permutation(jax.random.fold_in(own, 3), amount)
    donor, receiver = mixed[0:amount // 2 * 2:2], mixed[1:amount // 2 * 2:2]
    room = jnp.minimum(sizes[donor] - 1, limit - sizes[receiver]) // 2
    room = jnp.where((donor == sequence[0]) | (receiver == sequence[0]) | (sizes[receiver] == 0), 0, jnp.maximum(room, 0))
    passed = jax.random.randint(jax.random.fold_in(own, 4), (amount // 2,), 0, 1 << 20) % (room + 1)
    sizes = sizes.at[donor].add(-passed).at[receiver].add(passed)
    labels = jnp.searchsorted(jnp.cumsum(sizes), jnp.arange(rows * top), side="right").astype(jnp.int32)
    grid = labels.reshape(top, rows).T
    grid = grid[jax.random.permutation(jax.random.fold_in(own, 1), rows)]
    turn = jax.random.randint(jax.random.fold_in(own, 2), (rows, 1), 0, top)
    return jnp.take_along_axis(grid, (jnp.arange(top)[None, :] + turn) % top, axis=1)


def load_shares(amount, total, reach, slope, full):
    weights = [(1 << 20) // math.isqrt(rank ** slope) + 1 for rank in range(1, amount + 1)]
    largest = reach if full else min(reach, max(-(-total // amount), total * weights[0] // sum(weights)))
    least = 1 if total - largest >= amount - 1 else 0
    counts, rest = [largest] + [least] * (amount - 1), total - largest - least * (amount - 1)
    while rest > 0:
        free = [i for i in range(1, amount) if counts[i] < largest] or [i for i in range(1, amount) if counts[i] < reach]
        pool, budget = sum([weights[i] for i in free]), rest
        for i in free:
            more = min(reach - counts[i], max(1, budget * weights[i] // pool), rest)
            counts[i] = counts[i] + more
            rest = rest - more
    return np.array(counts)


def scatter_about(rng, shape, width, bound, pieces=(), kind=jnp.bfloat16):
    level = steps_of(rng, shape, pieces, -0.22, 0.18) if pieces else 1.0
    values = jax.random.normal(rng, shape, jnp.float32) * width * level
    return jnp.minimum(jnp.maximum(values, -bound), bound).astype(kind)


def setup_inputs(seed: int = 0) -> dict:
    key_of = jax.random.split(jax.random.key(seed), 19)
    mixer_in = draw_mixer_in(jax.random.fold_in(key_of[18], 71), 0)
    mixer_gain = jnp.clip(1.0 + 0.18 * jax.random.normal(key_of[1], (D,), jnp.float32), 0.1, 1.9)
    query_weight = draw_query_weight(jax.random.fold_in(key_of[18], 71), 0)
    key_weight = draw_key_weight(jax.random.fold_in(key_of[18], 71), 0)
    value_weight = scatter_about(key_of[4], (D, HEADS * VDIM), D ** -0.5, 0.125, ((1, 4),))
    head_lambda = jnp.clip(0.3 + 0.5 * jax.random.uniform(key_of[5], (HEADS,), jnp.float32) ** steps_of(key_of[5], (HEADS,), ((0, 4),), -0.2, 0.2), 0.3, 0.8)
    head_gain = jnp.clip(1.0 + 0.18 * jax.random.normal(key_of[6], (VDIM,), jnp.float32), 0.1, 1.9)
    out_weight = scatter_about(key_of[7], (HEADS * VDIM, D), (HEADS * VDIM) ** -0.5, 0.25, ((0, 4),))
    expert_in = scatter_about(key_of[8], (TOKENS, D), 1.0, 6.0, ((0, 32),))
    expert_gain = jnp.clip(1.0 + 0.18 * jax.random.normal(key_of[9], (D,), jnp.float32), 0.1, 1.9)
    routes_keys = jax.random.split(jax.random.fold_in(key_of[10], 1), TOKENS // TOK_DEV)
    routes_turns = jax.random.permutation(jax.random.fold_in(key_of[10], 3), TOKENS // TOK_DEV)
    routes = jax.vmap(lambda own, number: assign_block(jax.random.fold_in(key_of[10], 2), own, number, TOK_DEV, EXPERTS, TOPK, CAP, 1))(routes_keys, routes_turns).reshape((TOKENS, TOPK))
    route_weights = jnp.clip(jnp.exp(math.log(1.0) - 2.3025851 * jax.random.uniform(key_of[11], (TOKENS, TOPK), jnp.float32) ** steps_of(key_of[11], (TOKENS, TOPK), ((0, 32),), -0.2, 0.2)), 0.1, 1.0)
    gate_weight = scatter_about(key_of[12], (EXPERTS, D, FE), D ** -0.5, 0.125, ((0, 8),))
    up_weight = scatter_about(key_of[13], (EXPERTS, D, FE), D ** -0.5, 0.125, ((0, 8),))
    down_weight = scatter_about(key_of[14], (EXPERTS, FE, D), FE ** -0.5, 0.25, ((0, 8),))
    shared_gate = scatter_about(key_of[15], (D, FS), D ** -0.5, 0.125, ((1, 4),))
    shared_up = scatter_about(key_of[16], (D, FS), D ** -0.5, 0.125, ((1, 4),))
    shared_down = scatter_about(key_of[17], (FS, D), FS ** -0.5, 0.25, ((0, 4),))
    return {"mixer_in": mixer_in, "mixer_gain": mixer_gain, "query_weight": query_weight, "key_weight": key_weight, "value_weight": value_weight, "head_lambda": head_lambda, "head_gain": head_gain, "out_weight": out_weight, "expert_in": expert_in, "expert_gain": expert_gain, "routes": routes, "route_weights": route_weights, "gate_weight": gate_weight, "up_weight": up_weight, "down_weight": down_weight, "shared_gate": shared_gate, "shared_up": shared_up, "shared_down": shared_down}


EPS = 1e-06
ROUTED_SCALE = 2.5

def rms_rows(matrix, scales):
    values_in = matrix.astype(jnp.float32)
    inverse = lax.rsqrt(lax.optimization_barrier(jnp.mean(values_in * values_in, axis=-1, keepdims=True)) + EPS)
    return values_in * inverse * scales

def attend_block(query_rows, key_head, value_head, lambda_head, head_gain):
    reads = []
    for map_index in range(2):
        lower = map_index * HALF
        scores = jnp.dot(query_rows[:, lower:lower + HALF], key_head[:, lower:lower + HALF].T, preferred_element_type=jnp.float32) * HALF ** (-0.5)
        row_top = lax.optimization_barrier(jnp.max(scores, axis=1, keepdims=True))
        exponent = jnp.exp(scores - row_top)
        row_total = lax.optimization_barrier(jnp.sum(exponent, axis=1, keepdims=True))
        weights = exponent.astype(jnp.bfloat16)
        reads.append(jnp.dot(weights, value_head, preferred_element_type=jnp.float32) / row_total)
    difference = reads[0] - lambda_head * reads[1]
    return (rms_rows(difference, head_gain) * (1.0 - lambda_head)).astype(jnp.bfloat16)

def mixer_half(mixer_in, mixer_gain, query_weight, key_weight, value_weight, head_lambda, head_gain, out_weight):
    normed = rms_rows(mixer_in, mixer_gain).astype(jnp.bfloat16)
    queries = jnp.dot(normed, query_weight, preferred_element_type=jnp.float32).astype(jnp.bfloat16)
    keys_all = jnp.dot(normed, key_weight, preferred_element_type=jnp.float32).astype(jnp.bfloat16)
    values_all = jnp.dot(normed, value_weight, preferred_element_type=jnp.float32).astype(jnp.bfloat16)
    length = normed.shape[0]
    block_rows = math.gcd(length, 512)
    head_outputs = []
    for head_index in range(HEADS):
        lower = head_index * 2 * HALF
        query_head = queries[:, lower:lower + 2 * HALF].reshape(length // block_rows, block_rows, 2 * HALF)
        key_head = keys_all[:, lower:lower + 2 * HALF]
        value_head = values_all[:, head_index * VDIM:(head_index + 1) * VDIM]
        worker = partial(attend_block, key_head=key_head, value_head=value_head, lambda_head=head_lambda[head_index], head_gain=head_gain)
        head_outputs.append(lax.map(worker, query_head).reshape(length, VDIM))
    attended = jnp.concatenate(head_outputs, axis=1)
    group_cols = HEADS // N_TP * VDIM
    mixed_sum = jnp.zeros((length, D), jnp.float32)
    for group_index in range(N_TP):
        lower = group_index * group_cols
        piece_out = jnp.dot(attended[:, lower:lower + group_cols], out_weight[lower:lower + group_cols], preferred_element_type=jnp.float32).astype(jnp.bfloat16)
        mixed_sum = mixed_sum + lax.optimization_barrier(piece_out).astype(jnp.float32)
    return mixed_sum.astype(jnp.bfloat16)

def expert_half(expert_in, expert_gain, routes, route_weights, gate_weight, up_weight, down_weight, shared_gate, shared_up, shared_down):
    normed = rms_rows(expert_in, expert_gain).astype(jnp.bfloat16)
    length = normed.shape[0]
    shares = ROUTED_SCALE * route_weights / lax.optimization_barrier(jnp.sum(route_weights, axis=1, keepdims=True))
    group_cols = FS // N_TP
    shared_sum = jnp.zeros((length, D), jnp.float32)
    for group_index in range(N_TP):
        lower = group_index * group_cols
        gate_part = jnp.dot(normed, shared_gate[:, lower:lower + group_cols], preferred_element_type=jnp.float32)
        up_part = jnp.dot(normed, shared_up[:, lower:lower + group_cols], preferred_element_type=jnp.float32)
        hidden = (jax.nn.silu(gate_part) * up_part).astype(jnp.bfloat16)
        piece_out = jnp.dot(hidden, shared_down[lower:lower + group_cols], preferred_element_type=jnp.float32).astype(jnp.bfloat16)
        shared_sum = shared_sum + lax.optimization_barrier(piece_out).astype(jnp.float32)
    device_count = length // TOK_DEV
    assigned = TOK_DEV * TOPK
    blocks = routes.reshape(device_count, assigned).astype(jnp.int32)
    onehot = (blocks[:, :, None] == jnp.arange(EXPERTS, dtype=jnp.int32)[None, None, :]).astype(jnp.int32)
    slot_rank = lax.optimization_barrier(jnp.sum((jnp.cumsum(onehot, axis=1) - onehot) * onehot, axis=2)).astype(jnp.int32)
    column = jnp.arange(device_count, dtype=jnp.int32)[:, None] * CAP + slot_rank
    assign_ids = jnp.arange(device_count * assigned, dtype=jnp.int32).reshape(device_count, assigned)
    table = jnp.full((EXPERTS, device_count * CAP), length * TOPK, jnp.int32).at[blocks, column].set(assign_ids)
    padded_rows = jnp.concatenate([normed, jnp.zeros((1, D), jnp.bfloat16)], axis=0)
    padded_shares = jnp.concatenate([shares.reshape(-1), jnp.zeros((1,), jnp.float32)], axis=0)

    def one_expert(running, inputs):
        assign_row, gate_one, up_one, down_one = inputs
        tokens = (assign_row // TOPK).astype(jnp.int32)
        token_rows = padded_rows[tokens]
        gate_part = jnp.dot(token_rows, gate_one, preferred_element_type=jnp.float32)
        up_part = jnp.dot(token_rows, up_one, preferred_element_type=jnp.float32)
        hidden = (jax.nn.silu(gate_part) * up_part).astype(jnp.bfloat16)
        result = jnp.dot(hidden, down_one, preferred_element_type=jnp.float32).astype(jnp.bfloat16)
        weighted = lax.optimization_barrier(result).astype(jnp.float32) * padded_shares[assign_row][:, None]
        return (running.at[tokens].add(weighted), None)
    start_sum = jnp.zeros((length + 1, D), jnp.float32)
    routed, unused = lax.scan(one_expert, start_sum, (table, gate_weight, up_weight, down_weight))
    return (routed[:length] + shared_sum).astype(jnp.bfloat16)

def reference(mixer_in, mixer_gain, query_weight, key_weight, value_weight, head_lambda, head_gain, out_weight, expert_in, expert_gain, routes, route_weights, gate_weight, up_weight, down_weight, shared_gate, shared_up, shared_down):
    mixed_out = mixer_half(mixer_in, mixer_gain, query_weight, key_weight, value_weight, head_lambda, head_gain, out_weight)
    expert_out = expert_half(expert_in, expert_gain, routes, route_weights, gate_weight, up_weight, down_weight, shared_gate, shared_up, shared_down)
    return (mixed_out, expert_out)
```

```python
import functools
import math

import jax
import jax.numpy as jnp
from jax import lax
from jax.experimental import pallas as pl
from jax.experimental.pallas import tpu as pltpu
from jax.sharding import PartitionSpec as P

MESH = pl.DeviceIdType.MESH

EPS = 1e-06
ROUTED_SCALE = 2.5
VMEM_LIMIT = 53 * 1024 * 1024
PIECES = 4
HALVES = 2
SCHEDULE = (
    ("split", 0, 0),
    ("row", None, (-1, 0)),
    ("row", None, (1, 0)),
    ("proj1", None, None),
    ("row", None, (-1, 1)),
    ("wg", None, None),
    ("split", 1, -1),
    ("relay", None, None),
    ("exp", 1, 0),
    ("row", None, (2, 0)),
    ("row", None, (2, 1)),
    ("proj2", None, None),
    ("skv", (1, 0), (1, 0)),
    ("row", None, (1, 1)),
    ("split", 3, 2),
    ("fkv", None, (1, 0)),
    ("fkv", None, (-1, 0)),
    ("split", 2, 1),
    ("ch", (1, 0), None),
    ("far", None, None),
    ("att", 0, 1),
    ("skv", None, (-1, 0)),
    ("ch", (1, 1), None),
    ("exp", 3, 2),
    ("att", 2, -1),
    ("ch", (3, 0), None),
    ("exp", 2, 1),
    ("ch", (3, 1), None),
    ("fkv", None, (2, 0)),
    ("relaye", None, None),
    ("att", 1, 2),
    ("ch", (2, 0), None),
    ("exp", 0, -1),
    ("ch", (3, 2), None),
    ("ch", (3, 3), None),
    ("att", 3, 0),
    ("sendpart", None, None),
    ("ch", None, (2, 0)),
    ("ch", None, (2, 1)),
    ("ch", None, (1, 0)),
    ("ch", (2, 1), (2, 2)),
    ("ch", (2, 2), None),
    ("ch", None, (-1, 0)),
    ("relayw", None, None),
    ("ch", None, (-1, 1)),
    ("ch", None, (2, 3)),
    ("shared", None, None),
    ("ch", None, (1, 1)),
    ("ch", None, (-1, 2)),
    ("ch", (2, 3), None),
    ("ch", (1, 2), None),
    ("ch", (1, 3), None),
    ("ch", None, (1, 2)),
    ("ch", None, (-1, 3)),
    ("merge", None, None),
    ("ch", None, (1, 3)),
    ("gmix", None, None),
    ("gsh", None, None),
    ("final", None, None),
)


def rms_rows(matrix, scales):
    values_in = matrix.astype(jnp.float32)
    inverse = lax.rsqrt(jnp.mean(values_in * values_in, axis=-1, keepdims=True) + EPS)
    return values_in * inverse * scales


def on_device_plain(
    mixer_in,
    mixer_gain,
    query_weight,
    key_weight,
    value_weight,
    head_lambda,
    head_gain,
    out_weight,
    expert_in,
    expert_gain,
    routes,
    route_weights,
    gate_weight,
    up_weight,
    down_weight,
    shared_gate,
    shared_up,
    shared_down,
):
    model_width = mixer_in.shape[1]
    heads_dev = head_lambda.shape[0]
    value_dim = head_gain.shape[0]
    query_cols = query_weight.shape[1]
    half_dim = query_cols // (2 * heads_dev)
    normed_mixer = rms_rows(mixer_in, mixer_gain).astype(jnp.bfloat16)
    normed_expert = rms_rows(expert_in, expert_gain).astype(jnp.bfloat16)
    joined_weight = jnp.concatenate([query_weight, key_weight, value_weight], axis=1)
    projected = jnp.dot(
        lax.all_gather(normed_mixer, "tp", axis=0, tiled=True),
        joined_weight,
        preferred_element_type=jnp.float32,
    ).astype(jnp.bfloat16)
    block_rows = lax.all_gather(normed_expert, "tp", axis=0, tiled=True)
    gate_part = jnp.dot(block_rows, shared_gate, preferred_element_type=jnp.float32)
    up_part = jnp.dot(block_rows, shared_up, preferred_element_type=jnp.float32)
    shared_hidden = (jax.nn.silu(gate_part) * up_part).astype(jnp.bfloat16)
    gathered_rows = projected.shape[0]
    queries = projected[:, :query_cols].reshape(gathered_rows, heads_dev, 2, half_dim)
    key_rows = projected[:, query_cols : 2 * query_cols]
    value_rows = projected[:, 2 * query_cols :]
    scale_factor = half_dim ** (-0.5)

    def attend_block(running, key_block, value_block):
        top_now, total_now, acc_now = running
        span = key_block.shape[0]
        key_heads = key_block.reshape(span, heads_dev, 2, half_dim)
        value_heads = value_block.reshape(span, heads_dev, value_dim)
        scores = (
            jnp.einsum("qhcd,khcd->hcqk", queries, key_heads, preferred_element_type=jnp.float32)
            * scale_factor
        )
        top_next = jnp.maximum(top_now, jnp.max(scores, axis=-1))
        exponent = jnp.exp(scores - top_next[..., None])
        rescale = jnp.exp(top_now - top_next)
        total_next = total_now * rescale + jnp.sum(exponent, axis=-1)
        product = jnp.einsum(
            "hcqk,khe->hcqe",
            exponent.astype(jnp.bfloat16),
            value_heads,
            preferred_element_type=jnp.float32,
        )
        return (top_next, total_next, acc_now * rescale[..., None] + product)

    start_state = (
        jnp.full((heads_dev, 2, gathered_rows), -1e30, jnp.float32),
        jnp.zeros((heads_dev, 2, gathered_rows), jnp.float32),
        jnp.zeros((heads_dev, 2, gathered_rows, value_dim), jnp.float32),
    )
    key_piece = lax.all_gather(key_rows, "ep", axis=0, tiled=True)
    value_piece = lax.all_gather(value_rows, "ep", axis=0, tiled=True)
    span = key_piece.shape[0]
    block_len = math.gcd(span, 4 * gathered_rows)
    steps_count = span // block_len
    key_blocks = key_piece.reshape(steps_count, block_len, key_piece.shape[1])
    value_blocks = value_piece.reshape(steps_count, block_len, value_piece.shape[1])

    def step_once(state, blocks):
        return (attend_block(state, blocks[0], blocks[1]), None)

    result, unused = lax.scan(step_once, start_state, (key_blocks, value_blocks))
    top_all, total_all, acc_all = result
    read_out = acc_all / total_all[..., None]
    lambda_col = head_lambda[:, None, None]
    difference = read_out[:, 0] - lambda_col * read_out[:, 1]
    head_out = rms_rows(difference, head_gain) * (1.0 - lambda_col)
    attended = (
        jnp.transpose(head_out, (1, 0, 2))
        .reshape(gathered_rows, heads_dev * value_dim)
        .astype(jnp.bfloat16)
    )
    token_count = routes.shape[0]
    top_count = routes.shape[1]
    ep_count = lax.axis_size("ep")
    local_experts = gate_weight.shape[0]
    expert_count = ep_count * local_experts
    capacity = 2 * token_count * top_count // expert_count
    flat_routes = routes.reshape(-1)
    onehot = (flat_routes[:, None] == jnp.arange(expert_count, dtype=jnp.int32)[None, :]).astype(
        jnp.int32
    )
    earlier = jnp.cumsum(onehot, axis=0) - onehot
    slot_rank = jnp.sum(earlier * onehot, axis=1)
    slot_index = flat_routes * capacity + slot_rank
    owners = jnp.arange(token_count * top_count, dtype=jnp.int32) // top_count
    source = jnp.full((expert_count * capacity,), token_count, jnp.int32).at[slot_index].set(owners)
    padded = jnp.concatenate([normed_expert, jnp.zeros((1, model_width), jnp.bfloat16)], axis=0)
    outgoing = padded[source].reshape(ep_count, local_experts, capacity, model_width)
    arrived = lax.all_to_all(outgoing, "ep", split_axis=0, concat_axis=0, tiled=True)
    gate_part = jnp.einsum(
        "sxcd,xdf->sxcf", arrived, gate_weight, preferred_element_type=jnp.float32
    )
    up_part = jnp.einsum("sxcd,xdf->sxcf", arrived, up_weight, preferred_element_type=jnp.float32)
    hidden = (jax.nn.silu(gate_part) * up_part).astype(jnp.bfloat16)
    result = jnp.einsum(
        "sxcf,xfd->sxcd", hidden, down_weight, preferred_element_type=jnp.float32
    ).astype(jnp.bfloat16)
    returned = lax.all_to_all(result, "ep", split_axis=0, concat_axis=0, tiled=True)
    picked = returned.reshape(expert_count * capacity, model_width)[slot_index]
    picked = picked.reshape(token_count, top_count, model_width)
    shares = ROUTED_SCALE * route_weights / jnp.sum(route_weights, axis=1, keepdims=True)
    routed = jnp.sum(shares[:, :, None] * picked.astype(jnp.float32), axis=1)
    rows_here = attended
    mixer_sum = lax.psum_scatter(
        jnp.dot(rows_here, out_weight, preferred_element_type=jnp.float32).astype(jnp.bfloat16),
        "tp",
        scatter_dimension=0,
        tiled=True,
    )
    rows_here = shared_hidden
    shared_sum = lax.psum_scatter(
        jnp.dot(rows_here, shared_down, preferred_element_type=jnp.float32).astype(jnp.bfloat16),
        "tp",
        scatter_dimension=0,
        tiled=True,
    ).astype(jnp.float32)
    expert_out = (routed + shared_sum).astype(jnp.bfloat16)
    return (mixer_sum, expert_out)


def fused_kernel(
    n_ep,
    cap,
    mixer_in_hbm,
    mixer_gain_hbm,
    wq_hbm,
    wk_hbm,
    wv_hbm,
    head_lambda,
    head_gain_hbm,
    wo_hbm,
    expert_in_hbm,
    expert_gain_hbm,
    routes_hbm,
    weights_hbm,
    gate_hbm,
    up_hbm,
    down_hbm,
    sgate_hbm,
    sup_hbm,
    sdown_hbm,
    mixed_out,
    expert_out,
    mixer_in,
    mixer_gain,
    head_gain,
    expert_in,
    expert_gain,
    routes_t,
    weights_t,
    w_qkv,
    w_gate,
    w_up,
    w_down,
    w_sh,
    g_mix,
    g_exp,
    g_wo,
    g_wsd,
    outgoing,
    arrived,
    pair,
    back,
    combine,
    chain_out,
    chain_in,
    part_ref,
    temp_ref,
    kv_all,
    q_raw,
    q_far,
    q_two,
    read_out,
    read_in,
    lse_out,
    lse_in,
    att_mine,
    att_all,
    hid_mine,
    hid_all,
    top_ref,
    total_ref,
    acc_ref,
    z_rows,
    ranks,
    load_sem,
    tp_send,
    tp_recv,
    small_send,
    small_recv,
    rank_send,
    rank_recv,
    row_send,
    row_recv,
    kv_send,
    kv_recv,
    slots_send,
    slots_recv,
    back_send,
    back_recv,
    chain_send,
    chain_recv,
    twin_send,
    twin_recv,
):
    me = lax.axis_index("ep")
    tp = lax.axis_index("tp")
    near = tp + 1 - 2 * lax.rem(tp, 2)
    far = lax.rem(tp + 2, 4)
    cross = lax.rem(near + 2, 4)
    n_pair = n_ep // 2
    tokens, width = mixer_in.shape
    vdim = head_gain.shape[1]
    qcols = wq_hbm.shape[1]
    shid = sgate_hbm.shape[1]
    half = qcols // 2
    rows = 4 * tokens
    piece_cols = width // PIECES
    half_rows = tokens // HALVES

    line, low = me // 2, lax.rem(me, 2)
    twin = 2 * line + 1 - low
    last = n_pair - 1
    end_int = line // last + (last - line) // last
    is_end = end_int == 1
    is_inner = end_int == 0
    inward_way = line // (n_pair // 2)
    inward = 1 - 2 * inward_way

    small_pairs = (
        (mixer_in_hbm, mixer_in),
        (mixer_gain_hbm, mixer_gain),
        (expert_in_hbm, expert_in),
        (expert_gain_hbm, expert_gain),
        (routes_hbm, routes_t),
        (weights_hbm, weights_t),
        (head_gain_hbm, head_gain),
    )
    firsts = []
    for number, (origin, target) in enumerate(small_pairs):
        load = pltpu.make_async_copy(origin, target, load_sem.at[10 + number])
        load.start()
        firsts.append(load)

    def column_peer(hop):
        return 2 * lax.rem(line + hop, n_pair) + low

    barrier = pltpu.get_barrier_semaphore()
    for other in (near, far, cross):
        pl.semaphore_signal(barrier, inc=1, device_id=(me, other), device_id_type=MESH)
    pl.semaphore_signal(barrier, inc=1, device_id=(twin, tp), device_id_type=MESH)
    for hop in range(1, n_pair):
        pl.semaphore_signal(
            barrier, inc=1, device_id=(column_peer(hop), tp), device_id_type=MESH
        )

    pairs = (
        (wq_hbm, w_qkv.at[:, 0:qcols]),
        (wk_hbm, w_qkv.at[:, qcols : 2 * qcols]),
        (wv_hbm, w_qkv.at[:, 2 * qcols : 2 * qcols + vdim]),
        (sdown_hbm, g_wsd.at[tp]),
        (wo_hbm, g_wo.at[tp]),
        (gate_hbm.at[0], w_gate),
        (up_hbm.at[0], w_up),
        (down_hbm.at[0], w_down),
        (sgate_hbm, w_sh.at[:, 0:shid]),
        (sup_hbm, w_sh.at[:, shid : 2 * shid]),
    )
    loads = []
    for number, (origin, target) in enumerate(pairs):
        load = pltpu.make_async_copy(origin, target, load_sem.at[number])
        load.start()
        loads.append(load)

    def remote(origin, target, send_sem, recv_sem, device):
        return pltpu.make_async_remote_copy(
            src_ref=origin,
            dst_ref=target,
            send_sem=send_sem,
            recv_sem=recv_sem,
            device_id=device,
            device_id_type=MESH,
        )

    def tp_copy(buf, slot, other, number):
        place = buf.at[slot]
        return remote(place, place, tp_send.at[number], tp_recv.at[number], (me, other))

    def gather_start(buf, number):
        to_far = tp_copy(buf, tp, far, 3 * number)
        to_near = tp_copy(buf, tp, near, 3 * number + 1)
        to_far.start()
        to_near.start()
        return to_far, to_near

    def relay_start(buf, number, copies):
        copies[0].wait_recv()
        relay = tp_copy(buf, far, near, 3 * number + 2)
        relay.start()
        return relay

    def beside(way):
        return (2 * lax.rem(line + 1 - 2 * way + n_pair, n_pair) + low, tp)

    def row_copy(place, number, way):
        block = z_rows.at[place, pl.ds(number * half_rows, half_rows), :]
        return remote(
            block, block, row_send.at[way, place, number], row_recv.at[place, number], beside(way)
        )

    def kv_copy(place, way):
        block = kv_all.at[place]
        return remote(block, block, kv_send.at[way, place], kv_recv.at[place], beside(way))

    def rank_copy(hop):
        block = ranks.at[line]
        return remote(
            block, block, rank_send.at[hop], rank_recv.at[hop], (column_peer(hop), tp)
        )

    def slots_copy(place):
        return remote(
            outgoing.at[place],
            arrived.at[place, 1],
            slots_send.at[place],
            slots_recv.at[place],
            (twin, tp),
        )

    def back_copy(place, piece):
        return remote(
            back.at[place, piece],
            pair.at[place, piece, 1],
            back_send.at[place, piece],
            back_recv.at[place, piece],
            (twin, tp),
        )

    def chain_copy(place, piece, way):
        return remote(
            chain_out.at[place, piece],
            chain_in.at[way, place, piece],
            chain_send.at[place, piece],
            chain_recv.at[way, place, piece],
            beside(way),
        )

    def twin_copy(origin, target, number):
        return remote(origin, target, twin_send.at[number], twin_recv.at[number], (twin, tp))

    firsts[0].wait()
    firsts[1].wait()
    g_mix[tp] = rms_rows(mixer_in[...], mixer_gain[...]).astype(jnp.bfloat16)
    pl.semaphore_wait(barrier, n_pair + 3)
    mix_copies = gather_start(g_mix, 0)
    firsts[2].wait()
    firsts[3].wait()
    normed = rms_rows(expert_in[...], expert_gain[...]).astype(jnp.bfloat16)
    g_exp[tp] = normed
    z_rows[line] = normed
    for number in range(HALVES):
        row_copy(line, number, inward_way).start()

        @pl.when(is_inner)
        def _():
            row_copy(line, number, 1 - inward_way).start()

    exp_copies = gather_start(g_exp, 1)

    for number in range(4, 7):
        firsts[number].wait()
    expert_row = lax.broadcasted_iota(jnp.int32, (n_ep, tokens), 0)
    first, second = routes_t[0:1, :] == expert_row, routes_t[1:2, :] == expert_row
    named = jnp.logical_or(first, second)
    before = (
        lax.broadcasted_iota(jnp.int32, (tokens, tokens), 0)
        < lax.broadcasted_iota(jnp.int32, (tokens, tokens), 1)
    )
    rank = jnp.dot(
        jnp.where(named, 1.0, 0.0).astype(jnp.bfloat16),
        jnp.where(before, 1.0, 0.0).astype(jnp.bfloat16),
        preferred_element_type=jnp.float32,
    )
    scale = ROUTED_SCALE / (weights_t[0:1, :] + weights_t[1:2, :])
    share = jnp.where(first, weights_t[0:1, :] * scale, 0.0)
    share = share + jnp.where(second, weights_t[1:2, :] * scale, 0.0)
    ranks[line, 0:n_ep, :] = jnp.where(named, rank, -1.0)
    ranks[line, n_ep : 2 * n_ep, :] = share
    for hop in range(1, n_pair):
        rank_copy(hop).start()
    slot = lax.broadcasted_iota(jnp.int32, (cap, tokens), 0).astype(jnp.float32)

    top_ref[...] = jnp.full_like(top_ref, -1e30)
    total_ref[...] = jnp.zeros_like(total_ref)
    acc_ref[...] = jnp.zeros_like(acc_ref)
    held = {}

    def project(chip):
        block = g_mix[pl.ds(2 * chip, 2)].reshape(2 * tokens, width)
        out = jnp.dot(block, w_qkv[...], preferred_element_type=jnp.float32).astype(jnp.bfloat16)
        place = pl.ds(pl.multiple_of(2 * chip * tokens, 2 * tokens), 2 * tokens)
        kv_all[line, place, :] = out[:, qcols:]
        queries = (out[:, :qcols].astype(jnp.float32) * (half ** (-0.5))).astype(jnp.bfloat16)
        q_raw[place, :] = queries
        spread_halves(queries, place)

    def spread_halves(queries, place):
        wide = queries.astype(jnp.float32)
        lane = lax.broadcasted_iota(jnp.int32, wide.shape, 1)
        q_two[0, place, :] = jnp.where(lane < half, wide, 0.0).astype(jnp.bfloat16)
        q_two[1, place, :] = jnp.where(lane < half, 0.0, wide).astype(jnp.bfloat16)

    def task_split(place, at_end, at_inner):
        def wait_rank():
            rank_copy(lax.rem(line - place + n_pair, n_pair)).wait_recv()

        if at_end != 0:

            @pl.when(is_end)
            def _():
                for number in range(HALVES):
                    row_copy(place, number, 0).wait_recv()
                wait_rank()

        if at_inner != 0:

            @pl.when(is_inner)
            def _():
                wait_rank()

        wanted = [ranks[place, pl.ds(e, 1), :] == slot for e in (twin, me)]
        picks = jnp.concatenate([jnp.where(c, 1.0, 0.0) for c in wanted], axis=0)
        moved = jnp.dot(
            picks.astype(jnp.bfloat16), z_rows[place], preferred_element_type=jnp.float32
        ).astype(jnp.bfloat16)
        outgoing[place] = moved[:cap]
        slots_copy(place).start()
        arrived[place, 0] = moved[cap:]
        share_of = [ranks[place, pl.ds(n_ep + e, 1), :] for e in (twin, me)]
        weights = [jnp.where(c, g, 0.0) for c, g in zip(wanted, share_of)]
        weights = jnp.concatenate([weights[1], weights[0]], axis=0)
        high = weights.astype(jnp.bfloat16)
        combine[place, 0] = high
        combine[place, 1] = (weights - high.astype(jnp.float32)).astype(jnp.bfloat16)

    def task_exp(place, at_end, at_inner):
        if "experts" not in held:
            held["experts"] = True
            for number in range(5, 8):
                loads[number].wait()
        slots_copy(place).wait_recv()
        taken = arrived[place].reshape(2 * cap, width)
        gate_part = jnp.dot(taken, w_gate[...], preferred_element_type=jnp.float32)
        up_part = jnp.dot(taken, w_up[...], preferred_element_type=jnp.float32)
        hidden = (silu(gate_part) * up_part).astype(jnp.bfloat16)
        for piece in range(PIECES):
            answer = jnp.dot(
                hidden,
                w_down[:, piece * piece_cols : (piece + 1) * piece_cols],
                preferred_element_type=jnp.float32,
            ).astype(jnp.bfloat16)
            back[place, piece] = answer[cap:]
            back_copy(place, piece).start()
            pair[place, piece, 0] = answer[:cap]

    def combined(place, piece):
        back_copy(place, piece).wait_recv()
        answers = pair[place, piece].reshape(2 * cap, piece_cols)
        total = None
        for term in range(2):
            product = lax.dot_general(
                combine[place, term],
                answers,
                (((0,), (0,)), ((), ())),
                preferred_element_type=jnp.float32,
            )
            total = product if total is None else total + product
        return total

    def task_ch(place, piece, way, joins):
        value = combined(place, piece)
        if joins is None:
            chain_out[place, piece] = value.astype(jnp.bfloat16)
        elif joins is True:
            chain_copy(place, piece, way).wait_recv()
            chain_out[place, piece] = (
                value + chain_in[way, place, piece].astype(jnp.float32)
            ).astype(jnp.bfloat16)
        else:
            temp_ref[...] = value

            @pl.when(joins)
            def _():
                chain_copy(place, piece, way).wait_recv()
                temp_ref[...] = temp_ref[...] + chain_in[way, place, piece].astype(jnp.float32)

            chain_out[place, piece] = temp_ref[...].astype(jnp.bfloat16)

        chain_copy(place, piece, way).start()

    q_chunk = 2 * rows // 3

    def task_att(place, at_end, at_inner):
        if at_end != 0:

            @pl.when(is_end)
            def _():
                kv_copy(place, 0).wait_recv()

        keys = kv_all[place, :, 0:qcols]
        values_t = jnp.transpose(kv_all[place, :, qcols : qcols + vdim])
        ids = [(c, slice(r * q_chunk, (r + 1) * q_chunk)) for r in range(3) for c in range(2)]
        for c, part in ids:
            scores = lax.dot_general(
                keys,
                q_two[c, part, :],
                (((1,), (1,)), ((), ())),
                preferred_element_type=jnp.float32,
            )
            top_now = top_ref[c : c + 1, part]
            top_next = jnp.maximum(top_now, jnp.max(scores, axis=0, keepdims=True))
            exponent = jnp.exp(scores - top_next)
            rescale = jnp.exp(top_now - top_next)
            top_ref[c : c + 1, part] = top_next
            total_ref[c : c + 1, part] = total_ref[c : c + 1, part] * rescale + jnp.sum(
                exponent, axis=0, keepdims=True
            )
            acc_ref[c, :, part] = acc_ref[c, :, part] * rescale + jnp.dot(
                values_t, exponent.astype(jnp.bfloat16), preferred_element_type=jnp.float32
            )

    def spread(mine, everyone, base):
        copies = []
        for k, other in enumerate((near, far, cross)):
            copy = remote(
                mine.at[other],
                everyone.at[tp],
                small_send.at[base + k],
                small_recv.at[base + k],
                (me, other),
            )
            copy.start()
            copies.append(copy)
        everyone[tp] = mine[tp]
        return copies

    def grouped(rows_all, weight_all):
        total = None
        for g in range(4):
            piece = (
                jnp.dot(rows_all[g], weight_all[g], preferred_element_type=jnp.float32)
                .astype(jnp.bfloat16)
                .astype(jnp.float32)
            )
            total = piece if total is None else total + piece
        return total

    q_copy = twin_copy(q_raw, q_far, 0)
    read_copy = twin_copy(read_out, read_in, 1)
    lse_copy = twin_copy(lse_out, lse_in, 2)

    def task_wg():
        loads[3].wait()
        held["wsd"] = gather_start(g_wsd, 2)
        loads[4].wait()
        held["wo"] = gather_start(g_wo, 3)

    def task_proj1():
        for number in range(3):
            loads[number].wait()
        mix_copies[1].wait_recv()
        project(tp // 2)

    def task_relay():
        held["mix_relay"] = relay_start(g_mix, 0, mix_copies)

    def task_proj2():
        held["mix_relay"].wait_recv()
        project(far // 2)
        q_copy.start()

    def task_far():
        q_copy.wait_recv()
        spread_halves(q_far[...], slice(rows, 2 * rows))

    def task_relaye():
        held["exp_relay"] = relay_start(g_exp, 1, exp_copies)

    def task_shared():
        exp_copies[1].wait_recv()
        loads[8].wait()
        loads[9].wait()
        held["exp_relay"].wait_recv()
        both = jnp.dot(
            g_exp[...].reshape(rows, width), w_sh[...], preferred_element_type=jnp.float32
        )
        hid_mine[...] = (
            (silu(both[:, :shid]) * both[:, shid:]).astype(jnp.bfloat16).reshape(4, tokens, shid)
        )
        held["hid"] = spread(hid_mine, hid_all, 0)

    def task_relayw():
        held["wsd_relay"] = relay_start(g_wsd, 2, held["wsd"])
        held["wo_relay"] = relay_start(g_wo, 3, held["wo"])

    def task_gsh():
        held["wsd"][1].wait_recv()
        held["wsd_relay"].wait_recv()
        for copy in held["hid"]:
            copy.wait_recv()
        part_ref[...] = grouped(hid_all, g_wsd)

    def task_sendpart():
        place = slice(rows, 2 * rows)
        for c in range(2):
            read_out[c] = (acc_ref[c, :, place] / total_ref[c : c + 1, place]).astype(
                jnp.bfloat16
            )
            lse_out[c : c + 1, :] = top_ref[c : c + 1, place] + jnp.log(
                total_ref[c : c + 1, place]
            )
        read_copy.start()
        lse_copy.start()

    def task_merge():
        lam = head_lambda[0]
        lse_copy.wait_recv()
        read_copy.wait_recv()
        reads = []
        for c in range(2):
            total = total_ref[c : c + 1, 0:rows]
            lse_mine = top_ref[c : c + 1, 0:rows] + jnp.log(total)
            lse_far = lse_in[c : c + 1, :]
            best = jnp.maximum(lse_mine, lse_far)
            mine = jnp.exp(lse_mine - best)
            theirs = jnp.exp(lse_far - best)
            both = mine + theirs
            reads.append(
                acc_ref[c, :, 0:rows] * (mine / (both * total))
                + read_in[c].astype(jnp.float32) * (theirs / both)
            )
        difference = reads[0] - lam * reads[1]
        inverse = lax.rsqrt(jnp.mean(difference * difference, axis=0, keepdims=True) + EPS)
        head_out = jnp.transpose(difference * inverse) * head_gain[...] * (1.0 - lam)
        att_mine[...] = head_out.astype(jnp.bfloat16).reshape(4, tokens, vdim)
        held["att"] = spread(att_mine, att_all, 3)

    def task_gmix():
        held["wo"][1].wait_recv()
        held["wo_relay"].wait_recv()
        for copy in held["att"]:
            copy.wait_recv()
        mixed_out[...] = grouped(att_all, g_wo).astype(jnp.bfloat16)

    def task_final():
        for piece in range(PIECES):
            cols = slice(piece * piece_cols, (piece + 1) * piece_cols)
            chain_copy(line, piece, 1 - inward_way).wait_recv()
            value = (
                part_ref[:, cols]
                + combined(line, piece)
                + chain_in[1 - inward_way, line, piece].astype(jnp.float32)
            )
            part_ref[:, cols] = value

            @pl.when(is_inner)
            def _():
                chain_copy(line, piece, inward_way).wait_recv()
                part_ref[:, cols] = part_ref[:, cols] + chain_in[
                    inward_way, line, piece
                ].astype(jnp.float32)

            expert_out[:, cols] = part_ref[:, cols].astype(jnp.bfloat16)

    plain = {
        "wg": task_wg,
        "proj1": task_proj1,
        "relay": task_relay,
        "proj2": task_proj2,
        "far": task_far,
        "relaye": task_relaye,
        "shared": task_shared,
        "relayw": task_relayw,
        "gsh": task_gsh,
        "sendpart": task_sendpart,
        "merge": task_merge,
        "gmix": task_gmix,
        "final": task_final,
    }
    placed = {"split": task_split, "exp": task_exp, "att": task_att}

    def toward(hop):
        return inward_way if hop > 0 else 1 - inward_way

    def one_class(kind, hop, number):
        place = line + inward * hop
        if kind == "row":
            row_copy(place, number, 0).wait_recv()
            row_copy(place, number, toward(-hop)).start()
        elif kind == "skv":
            kv_copy(line, toward(hop)).start()
        else:
            kv_copy(place, 0).wait_recv()
            kv_copy(place, toward(-hop)).start()

    for kind, at_end, at_inner in SCHEDULE:
        if kind in plain:
            plain[kind]()
        elif kind in placed:
            hop = at_inner + (at_end - at_inner) * end_int
            placed[kind](line + inward * hop, at_end, at_inner)
        elif kind == "ch":
            if at_end is not None and at_inner is not None and at_inner[0] > 0:
                hop = at_inner[0] + (at_end[0] - at_inner[0]) * end_int
                piece = at_inner[1] + (at_end[1] - at_inner[1]) * end_int
                task_ch(line + inward * hop, piece, inward_way, is_inner)
            else:
                if at_end is not None:

                    @pl.when(is_end)
                    def _():
                        task_ch(line + inward * at_end[0], at_end[1], inward_way, None)

                if at_inner is not None:

                    @pl.when(is_inner)
                    def _():
                        task_ch(
                            line + inward * at_inner[0],
                            at_inner[1],
                            toward(at_inner[0]),
                            True,
                        )

        elif at_end is not None and at_end == at_inner:
            one_class(kind, *at_end)
        else:
            for chosen, spot in ((is_end, at_end), (is_inner, at_inner)):
                if spot is not None:

                    @pl.when(chosen)
                    def _():
                        one_class(kind, *spot)

    for copies in (mix_copies, exp_copies, held["wsd"], held["wo"]):
        for copy in copies:
            copy.wait_send()
    for name in ("mix_relay", "exp_relay", "wsd_relay", "wo_relay"):
        held[name].wait_send()
    for copies in (held["hid"], held["att"]):
        for copy in copies:
            copy.wait_send()
    for copy in (q_copy, read_copy, lse_copy):
        copy.wait_send()
    for hop in range(1, n_pair):
        rank_copy(hop).wait_send()
    for place in range(n_pair):
        slots_copy(place).wait_send()
        for piece in range(PIECES):
            back_copy(place, piece).wait_send()
    for number in range(HALVES):
        row_copy(line, number, inward_way).wait_send()
    kv_copy(line, inward_way).wait_send()
    for piece in range(PIECES):
        chain_copy(line + inward, piece, inward_way).wait_send()
        chain_copy(line + 2 * inward, piece, inward_way).wait_send()

    @pl.when(is_end)
    def _():
        for piece in range(PIECES):
            chain_copy(line + 3 * inward, piece, inward_way).wait_send()

    @pl.when(is_inner)
    def _():
        for piece in range(PIECES):
            chain_copy(line - inward, piece, 1 - inward_way).wait_send()
        kv_copy(line, 1 - inward_way).wait_send()
        for hop in (1, 2, -1):
            place = line + inward * hop
            kv_copy(place, toward(-hop)).wait_send()
            for number in range(HALVES):
                row_copy(place, number, toward(-hop)).wait_send()
        for number in range(HALVES):
            row_copy(line, number, 1 - inward_way).wait_send()


def silu(matrix):
    return matrix / (1.0 + jnp.exp(-matrix))


def on_device(*arguments):
    (mixer_in, mixer_gain, query_weight, key_weight, value_weight, head_lambda) = arguments[:6]
    (head_gain, out_weight, expert_in, expert_gain, routes, route_weights) = arguments[6:12]
    (gate_weight, up_weight, down_weight, shared_gate, shared_up, shared_down) = arguments[12:]
    n_ep, n_tp = lax.axis_size("ep"), lax.axis_size("tp")
    tokens, width = mixer_in.shape
    vdim, qcols, shid = head_gain.shape[0], query_weight.shape[1], shared_gate.shape[1]
    expert_hid = gate_weight.shape[2]
    cap = 2 * tokens * routes.shape[1] // n_ep
    fits = n_tp == 4 and n_ep % 2 == 0 and gate_weight.shape[0] == 1 and cap % 16 == 0
    fits = fits and routes.shape[1] == 2 and head_lambda.shape[0] == 1
    if not fits:
        return on_device_plain(*arguments)
    if n_ep != 8 or tokens % (16 * HALVES) or width % (128 * PIECES):
        return on_device_plain(*arguments)
    vmem = pl.BlockSpec(memory_space=pltpu.VMEM)
    hbm = pl.BlockSpec(memory_space=pltpu.HBM)
    smem = pl.BlockSpec(memory_space=pltpu.SMEM)
    rows, n_pair = n_tp * tokens, n_ep // 2
    half_type = jnp.bfloat16
    piece_cols = width // PIECES
    out_shape = jax.ShapeDtypeStruct((tokens, width), half_type)
    dma = pltpu.SemaphoreType.DMA
    scratch = [
        pltpu.VMEM((tokens, width), half_type),
        pltpu.VMEM((1, width), jnp.float32),
        pltpu.VMEM((1, vdim), jnp.float32),
        pltpu.VMEM((tokens, width), half_type),
        pltpu.VMEM((1, width), jnp.float32),
        pltpu.VMEM((2, tokens), jnp.int32),
        pltpu.VMEM((2, tokens), jnp.float32),
        pltpu.VMEM((width, 2 * qcols + vdim), half_type),
        pltpu.VMEM((width, expert_hid), half_type),
        pltpu.VMEM((width, expert_hid), half_type),
        pltpu.VMEM((expert_hid, width), half_type),
        pltpu.VMEM((width, 2 * shid), half_type),
        pltpu.VMEM((n_tp, tokens, width), half_type),
        pltpu.VMEM((n_tp, tokens, width), half_type),
        pltpu.VMEM((n_tp, vdim, width), half_type),
        pltpu.VMEM((n_tp, shid, width), half_type),
        pltpu.VMEM((n_pair, cap, width), half_type),
        pltpu.VMEM((n_pair, 2, cap, width), half_type),
        pltpu.VMEM((n_pair, PIECES, 2, cap, piece_cols), half_type),
        pltpu.VMEM((n_pair, PIECES, cap, piece_cols), half_type),
        pltpu.VMEM((n_pair, 2, 2 * cap, tokens), half_type),
        pltpu.VMEM((n_pair, PIECES, tokens, piece_cols), half_type),
        pltpu.VMEM((2, n_pair, PIECES, tokens, piece_cols), half_type),
        pltpu.VMEM((tokens, width), jnp.float32),
        pltpu.VMEM((tokens, piece_cols), jnp.float32),
        pltpu.VMEM((n_pair, rows, qcols + vdim), half_type),
        pltpu.VMEM((rows, qcols), half_type),
        pltpu.VMEM((rows, qcols), half_type),
        pltpu.VMEM((2, 2 * rows, qcols), half_type),
        pltpu.VMEM((2, vdim, rows), half_type),
        pltpu.VMEM((2, vdim, rows), half_type),
        pltpu.VMEM((2, rows), jnp.float32),
        pltpu.VMEM((2, rows), jnp.float32),
        pltpu.VMEM((n_tp, tokens, vdim), half_type),
        pltpu.VMEM((n_tp, tokens, vdim), half_type),
        pltpu.VMEM((n_tp, tokens, shid), half_type),
        pltpu.VMEM((n_tp, tokens, shid), half_type),
        pltpu.VMEM((2, 2 * rows), jnp.float32),
        pltpu.VMEM((2, 2 * rows), jnp.float32),
        pltpu.VMEM((2, vdim, 2 * rows), jnp.float32),
        pltpu.VMEM((n_pair, tokens, width), half_type),
        pltpu.VMEM((n_pair, 2 * n_ep, tokens), jnp.float32),
        dma((17,)),
        dma((12,)),
        dma((12,)),
        dma((6,)),
        dma((6,)),
        dma((n_pair,)),
        dma((n_pair,)),
        dma((2, n_pair, HALVES)),
        dma((n_pair, HALVES)),
        dma((2, n_pair)),
        dma((n_pair,)),
        dma((n_pair,)),
        dma((n_pair,)),
        dma((n_pair, PIECES)),
        dma((n_pair, PIECES)),
        dma((n_pair, PIECES)),
        dma((2, n_pair, PIECES)),
        dma((3,)),
        dma((3,)),
    ]
    return pl.pallas_call(
        functools.partial(fused_kernel, n_ep, cap),
        out_shape=(out_shape, out_shape),
        in_specs=[hbm] * 5 + [smem] + [hbm] * 12,
        out_specs=(vmem, vmem),
        scratch_shapes=scratch,
        compiler_params=pltpu.CompilerParams(
            collective_id=0, has_side_effects=True, vmem_limit_bytes=VMEM_LIMIT
        ),
    )(
        mixer_in,
        mixer_gain[None, :],
        query_weight,
        key_weight,
        value_weight,
        head_lambda,
        head_gain[None, :],
        out_weight,
        expert_in,
        expert_gain[None, :],
        routes.T,
        route_weights.T,
        gate_weight,
        up_weight,
        down_weight,
        shared_gate,
        shared_up,
        shared_down,
    )


def solution(mesh):
    in_specs = (
        P(("ep", "tp"), None),
        P(),
        P(None, "tp"),
        P(None, "tp"),
        P(None, "tp"),
        P("tp"),
        P(),
        P("tp", None),
        P(("ep", "tp"), None),
        P(),
        P(("ep", "tp"), None),
        P(("ep", "tp"), None),
        P("ep", None, None),
        P("ep", None, None),
        P("ep", None, None),
        P(None, "tp"),
        P(None, "tp"),
        P("tp", None),
    )
    out_specs = (P(("ep", "tp"), None), P(("ep", "tp"), None))
    return jax.shard_map(
        on_device, mesh=mesh, in_specs=in_specs, out_specs=out_specs, check_vma=False
    )
```
